256 devices in a mesh: grp: 2 (over z), ra: 16 (over y, core), cb: 8 (over x).
Axes of the slice: x: 8, y: 8, z: 2, core: 2. Of those that a mesh axis runs over, the one named last changes fastest.
The devices are a block of a 8x8x16 slice.
Arguments:
- tokens_in: bfloat16 [1024, 2048], P('grp', 'ra'), parts along dimension 0, may hold values from -40 to 40
- first_gain: float32 [2048], P('ra'), may hold values from 0.1 to 1.9
- first_gate: float32 [2048, 5632], P('ra', 'cb'), may hold values from -0.125 to 0.125
- first_gate_scale: float32 [5632], P('cb'), may hold values from 0.1 to 1.9
- first_up: float32 [2048, 5632], P('ra', 'cb'), may hold values from -0.125 to 0.125
- first_up_scale: float32 [5632], P('cb'), may hold values from 0.1 to 1.9
- first_down: float32 [5632, 2048], P('cb', 'ra'), may hold values from -0.078125 to 0.078125
- first_down_scale: float32 [2048], P('ra'), may hold values from 0.1 to 1.9
- second_gain: float32 [2048], P('ra'), may hold values from 0.1 to 1.9
- second_gate: float32 [2048, 5632], P('ra', 'cb'), may hold values from -0.125 to 0.125
- second_gate_scale: float32 [5632], P('cb'), may hold values from 0.1 to 1.9
- second_up: float32 [2048, 5632], P('ra', 'cb'), may hold values from -0.125 to 0.125
- second_up_scale: float32 [5632], P('cb'), may hold values from 0.1 to 1.9
- second_down: float32 [5632, 2048], P('cb', 'ra'), may hold values from -0.078125 to 0.078125
- second_down_scale: float32 [2048], P('ra'), may hold values from 0.1 to 1.9
Outputs:
- tokens_out: bfloat16 [1024, 2048], P('grp', 'ra'), parts along dimension 0
The draws below stay inside these ranges and needn't reach their ends.
There are 2 independent parts, one for each index of `grp`. The reference program is written for one: setup_inputs(seed, part) draws one part's arguments, and reference() takes and returns one part's arrays. A program takes and returns all parts, laid end to end along the dimension named above; an argument that names none is the same for every part. Nothing has to cross between parts.
All inputs are finite; a program needn't handle non-finite values.
Results may differ from the reference program's by a relative error of at most 0.04.
Values may be sent and summed in bfloat16 or wider, within the bound.
A program may use at most 64 MiB of HBM per device.

```python
import math
import jax
import jax.numpy as jnp
from jax import lax

D = 2048
FF = 5632
TOKENS = 512
FF_BLK = 704
N_CB = 8


def draw_tokens_in(key, part):
    first_key, second_key = jax.random.split(key)
    rows = jnp.exp(jax.random.uniform(first_key, (TOKENS, 1), jnp.float32, math.log(0.3), math.log(3.0)))
    base = jnp.clip(jax.random.normal(second_key, (TOKENS, D), jnp.float32), -4.0, 4.0)
    columns = 1.0 + 2.0 * jnp.arange(D, dtype=jnp.float32)[None, :] / (D - 1)
    return (base * rows * columns).astype(jnp.bfloat16)


def block_levels(stream_key, extent, shards, least, largest):
    def one(axis_at, blocks):
        heights = jax.random.uniform(jax.random.fold_in(jax.random.fold_in(stream_key, 6), axis_at), (blocks,), jnp.float32, least / len(shards), largest / len(shards))
        return jnp.repeat(jnp.exp(heights), extent[axis_at] // blocks).reshape((-1,) + (1,) * (len(extent) - axis_at - 1))

    level = one(*shards[0])
    for cut in shards[1:]:
        level = level * one(*cut)
    return level


def scatter_about(stream_key, extent, spread, reach, pieces=(), kind=jnp.bfloat16):
    drawn = spread * jax.random.normal(stream_key, extent, jnp.float32)
    if pieces:
        drawn = drawn * block_levels(stream_key, extent, pieces, -0.22, 0.18)
    return jnp.clip(drawn, -reach, reach).astype(kind)


def setup_inputs(seed: int = 0, part: int = 0) -> dict:
    seeds = jax.random.split(jax.random.key(seed), 16)
    own_keys = jax.random.split(jax.random.fold_in(seeds[15], part), 16)
    tokens_in = draw_tokens_in(jax.random.fold_in(jax.random.fold_in(seeds[15], part), 71), part)
    first_gain = jnp.clip(1.0 + 0.18 * jax.random.normal(seeds[1], (D,), jnp.float32), 0.1, 1.9)
    first_gate = scatter_about(seeds[2], (D, FF), D ** -0.5, 0.125, ((0, 16), (1, 8)), jnp.float32)
    first_gate_scale = jnp.clip(1.0 + 0.18 * jax.random.normal(seeds[3], (FF,), jnp.float32), 0.1, 1.9)
    first_up = scatter_about(seeds[4], (D, FF), D ** -0.5, 0.125, ((0, 16), (1, 8)), jnp.float32)
    first_up_scale = jnp.clip(1.0 + 0.18 * jax.random.normal(seeds[5], (FF,), jnp.float32), 0.1, 1.9)
    first_down = scatter_about(seeds[6], (FF, D), FF ** -0.5, 0.078125, ((0, 8), (1, 16)), jnp.float32)
    first_down_scale = jnp.clip(1.0 + 0.18 * jax.random.normal(seeds[7], (D,), jnp.float32), 0.1, 1.9)
    second_gain = jnp.clip(1.0 + 0.18 * jax.random.normal(seeds[8], (D,), jnp.float32), 0.1, 1.9)
    second_gate = scatter_about(seeds[9], (D, FF), D ** -0.5, 0.125, ((0, 16), (1, 8)), jnp.float32)
    second_gate_scale = jnp.clip(1.0 + 0.18 * jax.random.normal(seeds[10], (FF,), jnp.float32), 0.1, 1.9)
    second_up = scatter_about(seeds[11], (D, FF), D ** -0.5, 0.125, ((0, 16), (1, 8)), jnp.float32)
    second_up_scale = jnp.clip(1.0 + 0.18 * jax.random.normal(seeds[12], (FF,), jnp.float32), 0.1, 1.9)
    second_down = scatter_about(seeds[13], (FF, D), FF ** -0.5, 0.078125, ((0, 8), (1, 16)), jnp.float32)
    second_down_scale = jnp.clip(1.0 + 0.18 * jax.random.normal(seeds[14], (D,), jnp.float32), 0.1, 1.9)
    return {"tokens_in": tokens_in, "first_gain": first_gain, "first_gate": first_gate, "first_gate_scale": first_gate_scale, "first_up": first_up, "first_up_scale": first_up_scale, "first_down": first_down, "first_down_scale": first_down_scale, "second_gain": second_gain, "second_gate": second_gate, "second_gate_scale": second_gate_scale, "second_up": second_up, "second_up_scale": second_up_scale, "second_down": second_down, "second_down_scale": second_down_scale}


def half_step(acts, gain, gate_w, gate_s, up_w, up_s, down_w, down_s):
    acts_f = acts.astype(jnp.float32)
    mean_sq = lax.optimization_barrier(jnp.sum(acts_f * acts_f, axis=1, keepdims=True)) / D
    factor = lax.rsqrt(mean_sq + 1e-06)
    normed = (acts_f * gain).astype(jnp.bfloat16)
    gate = jnp.dot(normed, gate_w.astype(jnp.bfloat16), preferred_element_type=jnp.float32) * factor * gate_s
    up = jnp.dot(normed, up_w.astype(jnp.bfloat16), preferred_element_type=jnp.float32) * factor * up_s
    hidden = (jax.nn.silu(gate) * up).astype(jnp.bfloat16)
    blocks = hidden.reshape(TOKENS, N_CB, FF_BLK).astype(jnp.float32)
    weights = down_w.astype(jnp.bfloat16).astype(jnp.float32).reshape(N_CB, FF_BLK, D)
    partial_value = jnp.einsum('tcf,cfd->ctd', blocks, weights)
    partial_value = lax.optimization_barrier(partial_value.astype(jnp.bfloat16)).astype(jnp.float32)
    down = lax.optimization_barrier(jnp.sum(partial_value, axis=0)) * down_s
    return (0.5 * acts_f + 0.5 * down).astype(jnp.bfloat16)

def reference(tokens_in, first_gain, first_gate, first_gate_scale, first_up, first_up_scale, first_down, first_down_scale, second_gain, second_gate, second_gate_scale, second_up, second_up_scale, second_down, second_down_scale):
    middle = half_step(tokens_in, first_gain, first_gate, first_gate_scale, first_up, first_up_scale, first_down, first_down_scale)
    return half_step(middle, second_gain, second_gate, second_gate_scale, second_up, second_up_scale, second_down, second_down_scale)
```

```python
import functools

import jax
import jax.numpy as jnp
from jax import lax
from jax.experimental import pallas as pl
from jax.experimental.pallas import tpu as pltpu
from jax.sharding import PartitionSpec as P

MESH = pl.DeviceIdType.MESH
BF16 = jnp.bfloat16
F32 = jnp.float32
LANES = 128
CHUNKS = 2
Y_SCATTER, SQUARES, Y_GATHER, X_SCATTER, X_GATHER = range(5)


def kernel(
    n_y, n_x, chunks,
    x_hbm, gain1_hbm, gate1_hbm, gate1_s_hbm, up1_hbm, up1_s_hbm, down1_hbm, down1_s_hbm,
    gain2_hbm, gate2_hbm, gate2_s_hbm, up2_hbm, up2_s_hbm, down2_hbm, down2_s_hbm,
    out_hbm,
    acts, other, gate_f, up_f, down_f, scale_f, vecs, vecs_sib,
    w_gu, w_d, scale_gu,
    part, part_in, sq, sq_in, hid, down_part, down_in, out_buf,
    load_sem, sib_send, sib_recv, send_sem, recv_sem, out_sem,
):
    tokens, width = x_hbm.shape
    ff = gate_f.shape[2]
    half = tokens // 2
    rows = half // chunks
    y_rows, x_rows = rows // n_y, rows // n_x
    main = ff // LANES * LANES
    tail = ff - main

    ra, x_at = lax.axis_index("ra"), lax.axis_index("cb")
    core = lax.rem(ra, 2)
    y_at = ra // 2
    sibling = {"ra": ra + 1 - 2 * core}

    def y_peer(o):
        return {"ra": 2 * lax.rem(y_at + o, n_y) + core}

    def x_peer(o):
        return {"cb": lax.rem(x_at + o, n_x)}

    def x_cross(o):
        return {"ra": ra + 1 - 2 * core, "cb": lax.rem(x_at + o, n_x)}

    def by_distance(n):
        return sorted(range(1, n), key=lambda o: -min(o, n - o))

    mine = pl.ds(pl.multiple_of(half * core, half), half)
    theirs = pl.ds(pl.multiple_of(half * (1 - core), half), half)
    copies = [
        (x_hbm.at[theirs], other),
        (x_hbm.at[mine], acts.at[0, :, pl.ds(0, width)]),
        (gate1_hbm, gate_f.at[0]),
        (up1_hbm, up_f.at[0]),
        (gain1_hbm, vecs.at[0]),
        (gain2_hbm, vecs.at[1]),
        (down1_s_hbm, vecs.at[2]),
        (down2_s_hbm, vecs.at[3]),
        (gate1_s_hbm, scale_f.at[0]),
        (up1_s_hbm, scale_f.at[1]),
        (gate2_s_hbm, scale_f.at[2]),
        (up2_s_hbm, scale_f.at[3]),
        (down1_hbm, down_f.at[0]),
        (gate2_hbm, gate_f.at[1]),
        (up2_hbm, up_f.at[1]),
        (down2_hbm, down_f.at[1]),
    ]
    loads = [pltpu.make_async_copy(s, d, load_sem.at[i]) for i, (s, d) in enumerate(copies)]
    for load in loads:
        load.start()

    barrier = pltpu.get_barrier_semaphore()
    peers = [sibling]
    peers += [y_peer(o) for o in range(1, n_y)]
    peers += [x_peer(o) for o in range(1, n_x)]
    peers += [x_cross(o) for o in range(1, n_x)]
    for peer in peers:
        pl.semaphore_signal(barrier, inc=1, device_id=peer, device_id_type=MESH)

    def pack_gate_up(l):
        own = pl.ds(0, width)
        w_gu[l, own, 0:main] = gate_f[l, :, 0:main].astype(BF16)
        w_gu[l, own, main : 2 * main] = up_f[l, :, 0:main].astype(BF16)
        w_gu[l, own, 2 * main : 2 * ff] = jnp.concatenate(
            [gate_f[l, :, main:ff], up_f[l, :, main:ff]], axis=1
        ).astype(BF16)

    def pack_scales(l):
        scale_gu[l, :, 0:main] = scale_f[2 * l, :, 0:main]
        scale_gu[l, :, main : 2 * main] = scale_f[2 * l + 1, :, 0:main]
        scale_gu[l, :, 2 * main : 2 * ff] = jnp.concatenate(
            [scale_f[2 * l, :, main:ff], scale_f[2 * l + 1, :, main:ff]], axis=1
        )

    def pack_down(l):
        w_d[l, 0:ff, 0:width] = down_f[l].astype(BF16)
        w_d[l, ff : main + LANES, :] = jnp.zeros((main + LANES - ff, 2 * width), BF16)

    def to_sibling(i, src, dst):
        return pltpu.make_async_remote_copy(
            src_ref=src, dst_ref=dst, send_sem=sib_send.at[i], recv_sem=sib_recv.at[i],
            device_id=sibling, device_id_type=MESH,
        )

    def gate_up_swap(i, l):
        return to_sibling(i, w_gu.at[l, pl.ds(0, width)], w_gu.at[l, pl.ds(width, width)])

    def down_swap(i, l):
        return to_sibling(
            i, w_d.at[l, pl.ds(0, ff), pl.ds(0, width)], w_d.at[l, pl.ds(0, ff), pl.ds(width, width)]
        )

    swaps = [
        to_sibling(0, other, acts.at[0, :, pl.ds(width, width)]),
        to_sibling(1, vecs, vecs_sib),
        gate_up_swap(2, 0),
        down_swap(3, 0),
        gate_up_swap(4, 1),
        down_swap(5, 1),
    ]

    def send(l, phase, j, src, dst, peer):
        pltpu.make_async_remote_copy(
            src_ref=src, dst_ref=dst, send_sem=send_sem.at[l, phase, j],
            recv_sem=recv_sem.at[l, phase, j], device_id=peer, device_id_type=MESH,
        ).start()

    def await_recv(l, phase, j, ref):
        pltpu.make_async_remote_copy(
            src_ref=ref, dst_ref=ref, send_sem=send_sem.at[l, phase, j],
            recv_sem=recv_sem.at[l, phase, j], device_id=sibling, device_id_type=MESH,
        ).wait_recv()

    def await_send(l, phase, j, ref):
        pltpu.make_async_remote_copy(
            src_ref=ref, dst_ref=ref, send_sem=send_sem.at[l, phase, j],
            recv_sem=recv_sem.at[l, phase, j], device_id=sibling, device_id_type=MESH,
        ).wait_send()

    def pair(i):
        return jnp.concatenate([vecs[i], vecs_sib[i]], axis=1)

    def gate_up(l, j):
        at = pl.ds(j * rows, rows)
        a = acts[l, at, :]
        gram = lax.dot_general(a, a, (((1,), (1,)), ((), ())), preferred_element_type=F32)
        r = lax.broadcasted_iota(jnp.int32, (rows, rows), 0)
        c = lax.broadcasted_iota(jnp.int32, (rows, rows), 1)
        sq[l, j] = jnp.sum(jnp.where(r == c, gram, 0.0), axis=0, keepdims=True)
        for o in by_distance(n_y):
            send(l, SQUARES, j, sq.at[l, j], sq_in.at[l, j, o - 1], y_peer(o))
        normed = (a.astype(F32) * pair(l)).astype(BF16)
        for n in range(0, 2 * ff, 2 * LANES):
            cols = slice(n, min(n + 2 * LANES, 2 * ff))
            part[l, at, cols] = jnp.dot(
                normed, w_gu[l, :, cols], preferred_element_type=F32
            ).astype(BF16)
        for o in by_distance(n_y):
            to = lax.rem(y_at + o, n_y)
            src = part.at[l, pl.ds(pl.multiple_of(j * rows + to * y_rows, y_rows), y_rows)]
            send(l, Y_SCATTER, j, src, part_in.at[l, j, o - 1], y_peer(o))

    def hidden(l, j):
        await_recv(l, SQUARES, j, sq_in.at[l, j])
        total = sq[l, j]
        for o in range(1, n_y):
            total = total + sq_in[l, j, o - 1]
        r = lax.broadcasted_iota(jnp.int32, (y_rows, rows), 0)
        c = lax.broadcasted_iota(jnp.int32, (y_rows, rows), 1)
        column = jnp.sum(jnp.where(c == r + y_at * y_rows, total, 0.0), axis=1, keepdims=True)
        factor = lax.rsqrt(column / (2 * width * n_y) + 1e-06)
        await_recv(l, Y_SCATTER, j, part_in.at[l, j])
        own = pl.ds(pl.multiple_of(j * rows + y_at * y_rows, y_rows), y_rows)

        def summed(cols):
            value = part[l, own, cols].astype(F32)
            for o in range(1, n_y):
                value = value + part_in[l, j, o - 1, :, cols].astype(F32)
            return value * factor * scale_gu[l, :, cols]

        for n in range(0, main, LANES):
            gate = summed(slice(n, n + LANES))
            up = summed(slice(main + n, main + n + LANES))
            hid[l, own, n : n + LANES] = (gate / (1.0 + jnp.exp(-gate)) * up).astype(BF16)
        gate = summed(slice(2 * main, 2 * ff))
        up = pltpu.roll(gate, tail, 1)
        lane = lax.broadcasted_iota(jnp.int32, (y_rows, LANES), 1)
        last = jnp.where(lane < tail, gate / (1.0 + jnp.exp(-gate)) * up, 0.0)
        hid[l, own, main : main + LANES] = last.astype(BF16)
        for o in by_distance(n_y):
            send(l, Y_GATHER, j, hid.at[l, own], hid.at[l, own], y_peer(o))

    def down(l, j):
        at = pl.ds(j * rows, rows)
        await_recv(l, Y_GATHER, j, hid.at[l, pl.ds(0, rows - y_rows)])
        value = jnp.dot(hid[l, at, :], w_d[l], preferred_element_type=F32)
        down_part[l, at, :] = value.astype(BF16)
        for o in by_distance(n_x):
            to = lax.rem(x_at + o, n_x)
            src = down_part.at[l, pl.ds(pl.multiple_of(j * rows + to * x_rows, x_rows), x_rows)]
            send(l, X_SCATTER, j, src, down_in.at[l, j, o - 1], x_peer(o))

    def result(l, j):
        await_recv(l, X_SCATTER, j, down_in.at[l, j])
        own = pl.ds(pl.multiple_of(j * rows + x_at * x_rows, x_rows), x_rows)
        value = down_part[l, own, :].astype(F32)
        for o in range(1, n_x):
            value = value + down_in[l, j, o - 1].astype(F32)
        value = 0.5 * acts[l, own, :].astype(F32) + 0.5 * (value * pair(2 + l))
        value = value.astype(BF16)
        if l == 0:
            acts[1, own, :] = value
            for o in by_distance(n_x):
                send(l, X_GATHER, j, acts.at[1, own], acts.at[1, own], x_peer(o))
        else:
            place = pl.ds(
                pl.multiple_of(half * core + j * rows + x_at * x_rows, x_rows), x_rows
            )
            out_buf[0, place, :] = value[:, 0:width]
            down_part[0, own, width : 2 * width] = value[:, width : 2 * width]
            across = down_part.at[0, own, pl.ds(width, width)]
            for o in by_distance(n_x):
                send(l, X_GATHER, j, out_buf.at[0, place], out_buf.at[0, place], x_peer(o))
                send(l, X_GATHER, j, across, out_buf.at[0, place], x_cross(o))
            send(l, X_GATHER, j, across, out_buf.at[0, place], sibling)

    for i in range(12):
        loads[i].wait()
    pack_gate_up(0)
    pl.semaphore_wait(barrier, len(peers))
    for i in range(3):
        swaps[i].start()
    pack_scales(0)
    pack_scales(1)
    loads[12].wait()
    pack_down(0)
    swaps[3].start()
    for i in range(3):
        swaps[i].wait_recv()
    for j in range(chunks):
        gate_up(0, j)
    loads[13].wait()
    loads[14].wait()
    pack_gate_up(1)
    swaps[4].start()
    loads[15].wait()
    pack_down(1)
    swaps[5].start()
    for l in range(2):
        for j in range(chunks):
            if l == 1:
                await_recv(0, X_GATHER, j, acts.at[1, pl.ds(0, rows - x_rows)])
                if j == 0:
                    swaps[4].wait_recv()
                gate_up(1, j)
        for j in range(chunks):
            hidden(l, j)
        for j in range(chunks):
            if j == 0:
                swaps[3 + 2 * l].wait_recv()
            down(l, j)
        if l == 1:
            for j in range(chunks):
                await_send(0, X_SCATTER, j, down_in.at[0, j])
        for j in range(chunks):
            result(l, j)
    stores = []
    for j in range(chunks):
        await_recv(1, X_GATHER, j, out_buf.at[0, pl.ds(0, 2 * rows - x_rows)])
        for h in range(2):
            at = pl.ds(h * half + j * rows, rows)
            store = pltpu.make_async_copy(out_buf.at[0, at], out_hbm.at[at], out_sem.at[j, h])
            store.start()
            stores.append(store)
    for swap in swaps:
        swap.wait_send()
    for l in range(2):
        for j in range(chunks):
            await_send(l, Y_SCATTER, j, part_in.at[l, j])
            await_send(l, SQUARES, j, sq_in.at[l, j])
            await_send(l, Y_GATHER, j, hid.at[l, pl.ds(0, rows - y_rows)])
            if l == 1:
                await_send(1, X_SCATTER, j, down_in.at[1, j])
                await_send(1, X_GATHER, j, out_buf.at[0, pl.ds(0, 2 * rows - x_rows)])
            else:
                await_send(0, X_GATHER, j, acts.at[1, pl.ds(0, rows - x_rows)])
    for store in stores:
        store.wait()


def local(n_y, n_x, *args):
    x, gate, down = args[0], args[2], args[6]
    tokens, width = x.shape
    ff = gate.shape[1]
    padded = ff // LANES * LANES + LANES
    half = tokens // 2
    rows = half // CHUNKS
    y_rows, x_rows = rows // n_y, rows // n_x
    flat = [a.reshape(1, -1) if a.ndim == 1 else a for a in args]
    dma = pltpu.SemaphoreType.DMA
    return pl.pallas_call(
        functools.partial(kernel, n_y, n_x, CHUNKS),
        name="half_steps",
        out_shape=jax.ShapeDtypeStruct(x.shape, x.dtype),
        in_specs=[pl.BlockSpec(memory_space=pl.ANY)] * len(flat),
        out_specs=pl.BlockSpec(memory_space=pl.ANY),
        scratch_shapes=[
            pltpu.VMEM((2, half, 2 * width), BF16),
            pltpu.VMEM((half, width), BF16),
            pltpu.VMEM((2, width, ff), F32),
            pltpu.VMEM((2, width, ff), F32),
            pltpu.VMEM((2, ff, width), F32),
            pltpu.VMEM((4, 1, ff), F32),
            pltpu.VMEM((4, 1, width), F32),
            pltpu.VMEM((4, 1, width), F32),
            pltpu.VMEM((2, 2 * width, 2 * ff), BF16),
            pltpu.VMEM((2, padded, 2 * width), BF16),
            pltpu.VMEM((2, 1, 2 * ff), F32),
            pltpu.VMEM((2, half, 2 * ff), BF16),
            pltpu.VMEM((2, CHUNKS, n_y - 1, y_rows, 2 * ff), BF16),
            pltpu.VMEM((2, CHUNKS, 1, rows), F32),
            pltpu.VMEM((2, CHUNKS, n_y - 1, 1, rows), F32),
            pltpu.VMEM((2, half, padded), BF16),
            pltpu.VMEM((2, half, 2 * width), BF16),
            pltpu.VMEM((2, CHUNKS, n_x - 1, x_rows, 2 * width), BF16),
            pltpu.VMEM((1, tokens, width), BF16),
            dma((16,)),
            dma((6,)),
            dma((6,)),
            dma((2, 5, CHUNKS)),
            dma((2, 5, CHUNKS)),
            dma((CHUNKS, 2)),
        ],
        compiler_params=pltpu.CompilerParams(collective_id=0, has_side_effects=True),
    )(*flat)


def solution(mesh):
    n_y, n_x = mesh.shape["ra"] // 2, mesh.shape["cb"]
    layer = (P("ra"), P("ra", "cb"), P("cb"), P("ra", "cb"), P("cb"), P("cb", "ra"), P("ra"))
    return jax.shard_map(
        functools.partial(local, n_y, n_x),
        mesh=mesh,
        in_specs=(P("grp", "ra"), *layer, *layer),
        out_specs=P("grp", "ra"),
        check_vma=False,
    )
```

```python
import functools

import jax
import jax.numpy as jnp
from jax import lax
from jax.experimental import pallas as pl
from jax.experimental.pallas import tpu as pltpu
from jax.sharding import PartitionSpec as P

MESH = pl.DeviceIdType.MESH
BF16 = jnp.bfloat16
F32 = jnp.float32
LANES = 128
CHUNKS = 2
Y_SCATTER, SQUARES, Y_GATHER, X_SCATTER, X_GATHER = range(5)


def kernel(
    n_y, n_x, chunks,
    x_hbm, gain1_hbm, gate1_hbm, gate1_s_hbm, up1_hbm, up1_s_hbm, down1_hbm, down1_s_hbm,
    gain2_hbm, gate2_hbm, gate2_s_hbm, up2_hbm, up2_s_hbm, down2_hbm, down2_s_hbm,
    out_hbm,
    acts, other, gate_f, up_f, down_f, scale_0, scale_1, scale_2, scale_3, vecs, vecs_sib,
    w_gu, w_d, scale_gu,
    part, part_in, sq, sq_in, hid, down_part, down_in, out_buf,
    load_sem, sib_send, sib_recv, send_sem, recv_sem, out_sem,
):
    tokens, width = x_hbm.shape
    ff = gate_f.shape[1]
    half = tokens // 2
    rows = half // chunks
    y_rows, x_rows = rows // n_y, rows // n_x
    main = ff // LANES * LANES
    tail = ff - main

    ra, x_at = lax.axis_index("ra"), lax.axis_index("cb")
    core = lax.rem(ra, 2)
    y_at = ra // 2
    sibling = {"ra": ra + 1 - 2 * core}

    def y_peer(o):
        return {"ra": 2 * lax.rem(y_at + o, n_y) + core}

    def x_peer(o):
        return {"cb": lax.rem(x_at + o, n_x)}

    def x_cross(o):
        return {"ra": ra + 1 - 2 * core, "cb": lax.rem(x_at + o, n_x)}

    def by_distance(n):
        return sorted(range(1, n), key=lambda o: -min(o, n - o))

    mine = pl.ds(pl.multiple_of(half * core, half), half)
    theirs = pl.ds(pl.multiple_of(half * (1 - core), half), half)
    copies = [
        (x_hbm.at[theirs], other),
        (x_hbm.at[mine], acts.at[0, :, pl.ds(0, width)]),
        (gate1_hbm, gate_f.at[0]),
        (up1_hbm, up_f.at[0]),
        (gain1_hbm, vecs.at[0]),
        (gain2_hbm, vecs.at[1]),
        (down1_s_hbm, vecs.at[2]),
        (down2_s_hbm, vecs.at[3]),
        (gate1_s_hbm, scale_0),
        (up1_s_hbm, scale_1),
        (gate2_s_hbm, scale_2),
        (up2_s_hbm, scale_3),
        (down1_hbm, down_f.at[0]),
        (gate2_hbm, gate_f.at[1]),
        (up2_hbm, up_f.at[1]),
        (down2_hbm, down_f.at[1]),
    ]
    loads = [pltpu.make_async_copy(s, d, load_sem.at[i]) for i, (s, d) in enumerate(copies)]
    for load in loads:
        load.start()

    barrier = pltpu.get_barrier_semaphore()
    peers = [sibling]
    peers += [y_peer(o) for o in range(1, n_y)]
    peers += [x_peer(o) for o in range(1, n_x)]
    peers += [x_cross(o) for o in range(1, n_x)]
    for peer in peers:
        pl.semaphore_signal(barrier, inc=1, device_id=peer, device_id_type=MESH)

    def pack_gate_up(l):
        own = pl.ds(0, width)
        w_gu[l, 0:main, own] = gate_f[l, 0:main].astype(BF16)
        w_gu[l, main : 2 * main, own] = up_f[l, 0:main].astype(BF16)
        w_gu[l, 2 * main : main + ff, own] = gate_f[l, main:ff].astype(BF16)
        w_gu[l, main + ff : 2 * ff, own] = up_f[l, main:ff].astype(BF16)

    def pack_scales(l):
        gate_s, up_s = ((scale_0, scale_1), (scale_2, scale_3))[l]
        scale_gu[l, 0, 0:main] = gate_s[0:main]
        scale_gu[l, 0, main : 2 * main] = up_s[0:main]
        scale_gu[l, 0, 2 * main : main + ff] = gate_s[main:ff]
        scale_gu[l, 0, main + ff : 2 * ff] = up_s[main:ff]

    def pack_down(l):
        w_d[l, 0:ff, 0:width] = down_f[l].astype(BF16)
        w_d[l, ff : main + LANES, :] = jnp.zeros((main + LANES - ff, 2 * width), BF16)

    def to_sibling(i, src, dst):
        return pltpu.make_async_remote_copy(
            src_ref=src, dst_ref=dst, send_sem=sib_send.at[i], recv_sem=sib_recv.at[i],
            device_id=sibling, device_id_type=MESH,
        )

    def gate_up_swap(i, l):
        return to_sibling(i, w_gu.at[l, :, pl.ds(0, width)], w_gu.at[l, :, pl.ds(width, width)])

    def down_swap(i, l):
        return to_sibling(
            i, w_d.at[l, pl.ds(0, ff), pl.ds(0, width)], w_d.at[l, pl.ds(0, ff), pl.ds(width, width)]
        )

    swaps = [
        to_sibling(0, other, acts.at[0, :, pl.ds(width, width)]),
        to_sibling(1, vecs, vecs_sib),
        gate_up_swap(2, 0),
        down_swap(3, 0),
        gate_up_swap(4, 1),
        down_swap(5, 1),
    ]

    def send(l, phase, j, src, dst, peer):
        pltpu.make_async_remote_copy(
            src_ref=src, dst_ref=dst, send_sem=send_sem.at[l, phase, j],
            recv_sem=recv_sem.at[l, phase, j], device_id=peer, device_id_type=MESH,
        ).start()

    def await_recv(l, phase, j, ref):
        pltpu.make_async_remote_copy(
            src_ref=ref, dst_ref=ref, send_sem=send_sem.at[l, phase, j],
            recv_sem=recv_sem.at[l, phase, j], device_id=sibling, device_id_type=MESH,
        ).wait_recv()

    def await_send(l, phase, j, ref):
        pltpu.make_async_remote_copy(
            src_ref=ref, dst_ref=ref, send_sem=send_sem.at[l, phase, j],
            recv_sem=recv_sem.at[l, phase, j], device_id=sibling, device_id_type=MESH,
        ).wait_send()

    def pair(i):
        return jnp.concatenate([vecs[i], vecs_sib[i]], axis=1)

    def gate_up(l, j):
        at = pl.ds(j * rows, rows)
        a = acts[l, at, :]
        gram = lax.dot_general(a, a, (((1,), (1,)), ((), ())), preferred_element_type=F32)
        r = lax.broadcasted_iota(jnp.int32, (rows, rows), 0)
        c = lax.broadcasted_iota(jnp.int32, (rows, rows), 1)
        sq[l, j] = jnp.sum(jnp.where(r == c, gram, 0.0), axis=0, keepdims=True)
        for o in by_distance(n_y):
            send(l, SQUARES, j, sq.at[l, j], sq_in.at[l, j, o - 1], y_peer(o))
        normed = (a.astype(F32) * pair(l)).astype(BF16)
        for n in range(0, 2 * ff, 2 * LANES):
            cols = slice(n, min(n + 2 * LANES, 2 * ff))
            part[l, at, cols] = lax.dot_general(
                normed, w_gu[l, cols], (((1,), (1,)), ((), ())), preferred_element_type=F32
            ).astype(BF16)
        for o in by_distance(n_y):
            to = lax.rem(y_at + o, n_y)
            src = part.at[l, pl.ds(pl.multiple_of(j * rows + to * y_rows, y_rows), y_rows)]
            send(l, Y_SCATTER, j, src, part_in.at[l, j, o - 1], y_peer(o))

    def hidden(l, j):
        await_recv(l, SQUARES, j, sq_in.at[l, j])
        total = sq[l, j]
        for o in range(1, n_y):
            total = total + sq_in[l, j, o - 1]
        r = lax.broadcasted_iota(jnp.int32, (y_rows, rows), 0)
        c = lax.broadcasted_iota(jnp.int32, (y_rows, rows), 1)
        column = jnp.sum(jnp.where(c == r + y_at * y_rows, total, 0.0), axis=1, keepdims=True)
        factor = lax.rsqrt(column / (2 * width * n_y) + 1e-06)
        await_recv(l, Y_SCATTER, j, part_in.at[l, j])
        own = pl.ds(pl.multiple_of(j * rows + y_at * y_rows, y_rows), y_rows)

        def summed(cols):
            value = part[l, own, cols].astype(F32)
            for o in range(1, n_y):
                value = value + part_in[l, j, o - 1, :, cols].astype(F32)
            return value * factor * scale_gu[l, :, cols]

        for n in range(0, main, LANES):
            gate = summed(slice(n, n + LANES))
            up = summed(slice(main + n, main + n + LANES))
            hid[l, own, n : n + LANES] = (gate / (1.0 + jnp.exp(-gate)) * up).astype(BF16)
        gate = summed(slice(2 * main, 2 * ff))
        up = pltpu.roll(gate, tail, 1)
        lane = lax.broadcasted_iota(jnp.int32, (y_rows, LANES), 1)
        last = jnp.where(lane < tail, gate / (1.0 + jnp.exp(-gate)) * up, 0.0)
        hid[l, own, main : main + LANES] = last.astype(BF16)
        for o in by_distance(n_y):
            send(l, Y_GATHER, j, hid.at[l, own], hid.at[l, own], y_peer(o))

    def down(l, j):
        at = pl.ds(j * rows, rows)
        await_recv(l, Y_GATHER, j, hid.at[l, pl.ds(0, rows - y_rows)])
        value = jnp.dot(hid[l, at, :], w_d[l], preferred_element_type=F32)
        down_part[l, at, :] = value.astype(BF16)
        for o in by_distance(n_x):
            to = lax.rem(x_at + o, n_x)
            src = down_part.at[l, pl.ds(pl.multiple_of(j * rows + to * x_rows, x_rows), x_rows)]
            send(l, X_SCATTER, j, src, down_in.at[l, j, o - 1], x_peer(o))

    def result(l, j):
        await_recv(l, X_SCATTER, j, down_in.at[l, j])
        own = pl.ds(pl.multiple_of(j * rows + x_at * x_rows, x_rows), x_rows)
        value = down_part[l, own, :].astype(F32)
        for o in range(1, n_x):
            value = value + down_in[l, j, o - 1].astype(F32)
        value = 0.5 * acts[l, own, :].astype(F32) + 0.5 * (value * pair(2 + l))
        value = value.astype(BF16)
        if l == 0:
            acts[1, own, :] = value
            for o in by_distance(n_x):
                send(l, X_GATHER, j, acts.at[1, own], acts.at[1, own], x_peer(o))
        else:
            place = pl.ds(
                pl.multiple_of(half * core + j * rows + x_at * x_rows, x_rows), x_rows
            )
            out_buf[0, place, :] = value[:, 0:width]
            down_part[0, own, width : 2 * width] = value[:, width : 2 * width]
            across = down_part.at[0, own, pl.ds(width, width)]
            for o in by_distance(n_x):
                send(l, X_GATHER, j, out_buf.at[0, place], out_buf.at[0, place], x_peer(o))
                send(l, X_GATHER, j, across, out_buf.at[0, place], x_cross(o))
            send(l, X_GATHER, j, across, out_buf.at[0, place], sibling)

    for i in range(12):
        loads[i].wait()
    pack_gate_up(0)
    pl.semaphore_wait(barrier, len(peers))
    for i in range(3):
        swaps[i].start()
    pack_scales(0)
    pack_scales(1)
    loads[12].wait()
    pack_down(0)
    swaps[3].start()
    for i in range(3):
        swaps[i].wait_recv()
    for j in range(chunks):
        gate_up(0, j)
    loads[13].wait()
    loads[14].wait()
    pack_gate_up(1)
    swaps[4].start()
    loads[15].wait()
    pack_down(1)
    swaps[5].start()
    for l in range(2):
        for j in range(chunks):
            if l == 1:
                await_recv(0, X_GATHER, j, acts.at[1, pl.ds(0, rows - x_rows)])
                if j == 0:
                    swaps[4].wait_recv()
                gate_up(1, j)
        for j in range(chunks):
            hidden(l, j)
        for j in range(chunks):
            if j == 0:
                swaps[3 + 2 * l].wait_recv()
            down(l, j)
        if l == 1:
            for j in range(chunks):
                await_send(0, X_SCATTER, j, down_in.at[0, j])
        for j in range(chunks):
            result(l, j)
    stores = []
    for j in range(chunks):
        await_recv(1, X_GATHER, j, out_buf.at[0, pl.ds(0, 2 * rows - x_rows)])
        for h in range(2):
            at = pl.ds(h * half + j * rows, rows)
            store = pltpu.make_async_copy(out_buf.at[0, at], out_hbm.at[at], out_sem.at[j, h])
            store.start()
            stores.append(store)
    for swap in swaps:
        swap.wait_send()
    for l in range(2):
        for j in range(chunks):
            await_send(l, Y_SCATTER, j, part_in.at[l, j])
            await_send(l, SQUARES, j, sq_in.at[l, j])
            await_send(l, Y_GATHER, j, hid.at[l, pl.ds(0, rows - y_rows)])
            if l == 1:
                await_send(1, X_SCATTER, j, down_in.at[1, j])
                await_send(1, X_GATHER, j, out_buf.at[0, pl.ds(0, 2 * rows - x_rows)])
            else:
                await_send(0, X_GATHER, j, acts.at[1, pl.ds(0, rows - x_rows)])
    for store in stores:
        store.wait()


def local(n_y, n_x, *args):
    x, gate, down = args[0], args[2], args[6]
    tokens, width = x.shape
    ff = gate.shape[1]
    padded = ff // LANES * LANES + LANES
    half = tokens // 2
    rows = half // CHUNKS
    y_rows, x_rows = rows // n_y, rows // n_x
    flat = [a.reshape(1, -1) if a.shape == (width,) else a for a in args]
    for i in (2, 4, 9, 11):
        flat[i] = args[i].T
    dma = pltpu.SemaphoreType.DMA
    return pl.pallas_call(
        functools.partial(kernel, n_y, n_x, CHUNKS),
        name="half_steps",
        out_shape=jax.ShapeDtypeStruct(x.shape, x.dtype),
        in_specs=[pl.BlockSpec(memory_space=pl.ANY)] * len(flat),
        out_specs=pl.BlockSpec(memory_space=pl.ANY),
        scratch_shapes=[
            pltpu.VMEM((2, half, 2 * width), BF16),
            pltpu.VMEM((half, width), BF16),
            pltpu.VMEM((2, ff, width), F32),
            pltpu.VMEM((2, ff, width), F32),
            pltpu.VMEM((2, ff, width), F32),
            pltpu.VMEM((ff,), F32),
            pltpu.VMEM((ff,), F32),
            pltpu.VMEM((ff,), F32),
            pltpu.VMEM((ff,), F32),
            pltpu.VMEM((4, 1, width), F32),
            pltpu.VMEM((4, 1, width), F32),
            pltpu.VMEM((2, 2 * ff, 2 * width), BF16),
            pltpu.VMEM((2, padded, 2 * width), BF16),
            pltpu.VMEM((2, 1, 2 * ff), F32),
            pltpu.VMEM((2, half, 2 * ff), BF16),
            pltpu.VMEM((2, CHUNKS, n_y - 1, y_rows, 2 * ff), BF16),
            pltpu.VMEM((2, CHUNKS, 1, rows), F32),
            pltpu.VMEM((2, CHUNKS, n_y - 1, 1, rows), F32),
            pltpu.VMEM((2, half, padded), BF16),
            pltpu.VMEM((2, half, 2 * width), BF16),
            pltpu.VMEM((2, CHUNKS, n_x - 1, x_rows, 2 * width), BF16),
            pltpu.VMEM((1, tokens, width), BF16),
            dma((16,)),
            dma((6,)),
            dma((6,)),
            dma((2, 5, CHUNKS)),
            dma((2, 5, CHUNKS)),
            dma((CHUNKS, 2)),
        ],
        compiler_params=pltpu.CompilerParams(collective_id=0, has_side_effects=True),
    )(*flat)


def solution(mesh):
    n_y, n_x = mesh.shape["ra"] // 2, mesh.shape["cb"]
    layer = (P("ra"), P("ra", "cb"), P("cb"), P("ra", "cb"), P("cb"), P("cb", "ra"), P("ra"))
    return jax.shard_map(
        functools.partial(local, n_y, n_x),
        mesh=mesh,
        in_specs=(P("grp", "ra"), *layer, *layer),
        out_specs=P("grp", "ra"),
        check_vma=False,
    )
```

```python
import functools

import jax
import jax.numpy as jnp
from jax import lax
from jax.experimental import pallas as pl
from jax.experimental.pallas import tpu as pltpu
from jax.sharding import PartitionSpec as P

MESH = pl.DeviceIdType.MESH
BF16 = jnp.bfloat16
F32 = jnp.float32
LANES = 128
CHUNKS = 2
SQUARES, FOR_THREE, FOR_FOUR, FOR_ONE, FOR_TWO, FROM_TWO, FROM_REST, X_SCATTER, X_GATHER = range(9)


def kernel(
    n_y, n_x, chunks,
    x_hbm, gain1_hbm, gate1_hbm, gate1_s_hbm, up1_hbm, up1_s_hbm, down1_hbm, down1_s_hbm,
    gain2_hbm, gate2_hbm, gate2_s_hbm, up2_hbm, up2_s_hbm, down2_hbm, down2_s_hbm,
    out_hbm,
    acts, other, gate_f, up_f, down_f, scale_0, scale_1, scale_2, scale_3, vecs, vecs_sib,
    w_gu, w_d, scale_gu,
    part, in_three, in_four, in_one, in_two, out_two, sq, sq_in, hid, down_part, down_in, out_buf,
    load_sem, sib_send, sib_recv, send_sem, recv_sem, out_sem,
):
    tokens, width = x_hbm.shape
    ff = gate_f.shape[1]
    half = tokens // 2
    rows = half // chunks
    y_rows, x_rows = rows // n_y, rows // n_x
    main = ff // LANES * LANES
    tail = ff - main

    ra, x_at = lax.axis_index("ra"), lax.axis_index("cb")
    core = lax.rem(ra, 2)
    y_at = ra // 2
    sibling = {"ra": ra + 1 - 2 * core}

    def y_peer(o):
        return {"ra": 2 * lax.rem(y_at + o + n_y, n_y) + core}

    def x_peer(o):
        return {"cb": lax.rem(x_at + o, n_x)}

    def x_cross(o):
        return {"ra": ra + 1 - 2 * core, "cb": lax.rem(x_at + o, n_x)}

    def y_share(j, o):
        return pl.ds(pl.multiple_of(j * rows + lax.rem(y_at + o + n_y, n_y) * y_rows, y_rows), y_rows)

    part_halves = (pl.ds(0, main), pl.ds(main, 2 * ff - main))
    hid_half = (main + LANES) // 2 // LANES * LANES
    hid_halves = (pl.ds(0, hid_half), pl.ds(hid_half, main + LANES - hid_half))

    def by_distance(n):
        return sorted(range(1, n), key=lambda o: -min(o, n - o))

    mine = pl.ds(pl.multiple_of(half * core, half), half)
    theirs = pl.ds(pl.multiple_of(half * (1 - core), half), half)
    copies = [
        (x_hbm.at[theirs], other),
        (x_hbm.at[mine], acts.at[0, :, pl.ds(0, width)]),
        (gate1_hbm, gate_f.at[0]),
        (up1_hbm, up_f.at[0]),
        (gain1_hbm, vecs.at[0]),
        (gain2_hbm, vecs.at[1]),
        (down1_s_hbm, vecs.at[2]),
        (down2_s_hbm, vecs.at[3]),
        (gate1_s_hbm, scale_0),
        (up1_s_hbm, scale_1),
        (gate2_s_hbm, scale_2),
        (up2_s_hbm, scale_3),
        (down1_hbm, down_f.at[0]),
        (gate2_hbm, gate_f.at[1]),
        (up2_hbm, up_f.at[1]),
        (down2_hbm, down_f.at[1]),
    ]
    loads = [pltpu.make_async_copy(s, d, load_sem.at[i]) for i, (s, d) in enumerate(copies)]
    for load in loads:
        load.start()

    barrier = pltpu.get_barrier_semaphore()
    peers = [sibling]
    peers += [y_peer(o) for o in range(1, n_y)]
    peers += [x_peer(o) for o in range(1, n_x)]
    peers += [x_cross(o) for o in range(1, n_x)]
    for peer in peers:
        pl.semaphore_signal(barrier, inc=1, device_id=peer, device_id_type=MESH)

    def pack_gate_up(l):
        own = pl.ds(0, width)
        w_gu[l, 0:main, own] = gate_f[l, 0:main].astype(BF16)
        w_gu[l, main : 2 * main, own] = up_f[l, 0:main].astype(BF16)
        w_gu[l, 2 * main : main + ff, own] = gate_f[l, main:ff].astype(BF16)
        w_gu[l, main + ff : 2 * ff, own] = up_f[l, main:ff].astype(BF16)

    def pack_scales(l):
        gate_s, up_s = ((scale_0, scale_1), (scale_2, scale_3))[l]
        scale_gu[l, 0, 0:main] = gate_s[0:main]
        scale_gu[l, 0, main : 2 * main] = up_s[0:main]
        scale_gu[l, 0, 2 * main : main + ff] = gate_s[main:ff]
        scale_gu[l, 0, main + ff : 2 * ff] = up_s[main:ff]

    def pack_down(l):
        w_d[l, 0:ff, 0:width] = down_f[l].astype(BF16)
        w_d[l, ff : main + LANES, :] = jnp.zeros((main + LANES - ff, 2 * width), BF16)

    def to_sibling(i, src, dst):
        return pltpu.make_async_remote_copy(
            src_ref=src, dst_ref=dst, send_sem=sib_send.at[i], recv_sem=sib_recv.at[i],
            device_id=sibling, device_id_type=MESH,
        )

    def gate_up_swap(i, l):
        return to_sibling(i, w_gu.at[l, :, pl.ds(0, width)], w_gu.at[l, :, pl.ds(width, width)])

    def down_swap(i, l):
        return to_sibling(
            i, w_d.at[l, pl.ds(0, ff), pl.ds(0, width)], w_d.at[l, pl.ds(0, ff), pl.ds(width, width)]
        )

    swaps = [
        to_sibling(0, other, acts.at[0, :, pl.ds(width, width)]),
        to_sibling(1, vecs, vecs_sib),
        gate_up_swap(2, 0),
        down_swap(3, 0),
        gate_up_swap(4, 1),
        down_swap(5, 1),
    ]

    def send(l, phase, j, src, dst, peer):
        pltpu.make_async_remote_copy(
            src_ref=src, dst_ref=dst, send_sem=send_sem.at[l, phase, j],
            recv_sem=recv_sem.at[l, phase, j], device_id=peer, device_id_type=MESH,
        ).start()

    def await_recv(l, phase, j, ref):
        pltpu.make_async_remote_copy(
            src_ref=ref, dst_ref=ref, send_sem=send_sem.at[l, phase, j],
            recv_sem=recv_sem.at[l, phase, j], device_id=sibling, device_id_type=MESH,
        ).wait_recv()

    def await_send(l, phase, j, ref):
        pltpu.make_async_remote_copy(
            src_ref=ref, dst_ref=ref, send_sem=send_sem.at[l, phase, j],
            recv_sem=recv_sem.at[l, phase, j], device_id=sibling, device_id_type=MESH,
        ).wait_send()

    def pair(i):
        return jnp.concatenate([vecs[i], vecs_sib[i]], axis=1)

    def gate_up(l, j):
        at = pl.ds(j * rows, rows)
        a = acts[l, at, :]
        gram = lax.dot_general(a, a, (((1,), (1,)), ((), ())), preferred_element_type=F32)
        r = lax.broadcasted_iota(jnp.int32, (rows, rows), 0)
        c = lax.broadcasted_iota(jnp.int32, (rows, rows), 1)
        sq[l, j] = jnp.sum(jnp.where(r == c, gram, 0.0), axis=0, keepdims=True)
        for o in by_distance(n_y):
            send(l, SQUARES, j, sq.at[l, j], sq_in.at[l, j, o - 1], y_peer(o))
        normed = (a.astype(F32) * pair(l)).astype(BF16)
        for n in range(0, 2 * ff, 2 * LANES):
            cols = slice(n, min(n + 2 * LANES, 2 * ff))
            part[l, at, cols] = lax.dot_general(
                normed, w_gu[l, cols], (((1,), (1,)), ((), ())), preferred_element_type=F32
            ).astype(BF16)
        for s, sign in enumerate((1, -1)):
            cols = part_halves[s]
            send(l, FOR_FOUR, j, part.at[l, y_share(j, 4), cols], in_four.at[l, j, :, cols], y_peer(2 * sign))
        for s, sign in enumerate((1, -1)):
            send(l, FOR_THREE, j, part.at[l, y_share(j, 3 * sign)], in_three.at[l, j, s], y_peer(sign))
        for s, sign in enumerate((1, -1)):
            send(l, FOR_ONE, j, part.at[l, y_share(j, sign)], in_one.at[l, j, s], y_peer(sign))

    def combine(l, j):
        await_recv(l, FOR_THREE, j, in_three.at[l, j])
        await_recv(l, FOR_FOUR, j, in_four.at[l, j])
        for s, sign in enumerate((1, -1)):
            at = y_share(j, 2 * sign)
            for h, cols in enumerate(part_halves):
                value = part[l, at, cols].astype(F32) + in_three[l, j, s, :, cols].astype(F32)
                if h == s:
                    value = value + in_four[l, j, :, cols].astype(F32)
                out_two[l, j, s, :, cols] = value.astype(BF16)
            send(l, FOR_TWO, j, out_two.at[l, j, s], in_two.at[l, j, s], y_peer(2 * sign))

    def hidden(l, j):
        await_recv(l, SQUARES, j, sq_in.at[l, j])
        total = sq[l, j]
        for o in range(1, n_y):
            total = total + sq_in[l, j, o - 1]
        r = lax.broadcasted_iota(jnp.int32, (y_rows, rows), 0)
        c = lax.broadcasted_iota(jnp.int32, (y_rows, rows), 1)
        column = jnp.sum(jnp.where(c == r + y_at * y_rows, total, 0.0), axis=1, keepdims=True)
        factor = lax.rsqrt(column / (2 * width * n_y) + 1e-06)
        await_recv(l, FOR_ONE, j, in_one.at[l, j])
        await_recv(l, FOR_TWO, j, in_two.at[l, j])
        own = y_share(j, 0)

        def summed(cols):
            value = part[l, own, cols].astype(F32)
            for s in range(2):
                value = value + in_one[l, j, s, :, cols].astype(F32)
                value = value + in_two[l, j, s, :, cols].astype(F32)
            return value * factor * scale_gu[l, :, cols]

        for n in range(0, main, LANES):
            gate = summed(slice(n, n + LANES))
            up = summed(slice(main + n, main + n + LANES))
            hid[l, own, n : n + LANES] = (gate / (1.0 + jnp.exp(-gate)) * up).astype(BF16)
        gate = summed(slice(2 * main, 2 * ff))
        up = pltpu.roll(gate, tail, 1)
        lane = lax.broadcasted_iota(jnp.int32, (y_rows, LANES), 1)
        last = jnp.where(lane < tail, gate / (1.0 + jnp.exp(-gate)) * up, 0.0)
        hid[l, own, main : main + LANES] = last.astype(BF16)
        for sign in (1, -1):
            send(l, FROM_TWO, j, hid.at[l, own], hid.at[l, own], y_peer(2 * sign))
        for sign in (1, -1):
            send(l, FROM_REST, j, hid.at[l, own], hid.at[l, own], y_peer(sign))

    def forward(l, j):
        await_recv(l, FROM_TWO, j, hid.at[l, pl.ds(0, 2 * y_rows)])
        for s, sign in enumerate((1, -1)):
            half_share = hid.at[l, y_share(j, -2 * sign), hid_halves[s]]
            send(l, FROM_REST, j, half_share, half_share, y_peer(2 * sign))
        for sign in (1, -1):
            share = hid.at[l, y_share(j, -2 * sign)]
            send(l, FROM_REST, j, share, share, y_peer(sign))

    def down(l, j):
        at = pl.ds(j * rows, rows)
        await_recv(l, FROM_REST, j, hid.at[l, pl.ds(0, 5 * y_rows)])
        value = jnp.dot(hid[l, at, :], w_d[l], preferred_element_type=F32)
        down_part[l, at, :] = value.astype(BF16)
        for o in by_distance(n_x):
            to = lax.rem(x_at + o, n_x)
            src = down_part.at[l, pl.ds(pl.multiple_of(j * rows + to * x_rows, x_rows), x_rows)]
            send(l, X_SCATTER, j, src, down_in.at[l, j, o - 1], x_peer(o))

    def result(l, j):
        await_recv(l, X_SCATTER, j, down_in.at[l, j])
        own = pl.ds(pl.multiple_of(j * rows + x_at * x_rows, x_rows), x_rows)
        value = down_part[l, own, :].astype(F32)
        for o in range(1, n_x):
            value = value + down_in[l, j, o - 1].astype(F32)
        value = 0.5 * acts[l, own, :].astype(F32) + 0.5 * (value * pair(2 + l))
        value = value.astype(BF16)
        if l == 0:
            acts[1, own, :] = value
            for o in by_distance(n_x):
                send(l, X_GATHER, j, acts.at[1, own], acts.at[1, own], x_peer(o))
        else:
            place = pl.ds(
                pl.multiple_of(half * core + j * rows + x_at * x_rows, x_rows), x_rows
            )
            out_buf[0, place, :] = value[:, 0:width]
            down_part[0, own, width : 2 * width] = value[:, width : 2 * width]
            across = down_part.at[0, own, pl.ds(width, width)]
            for o in by_distance(n_x):
                send(l, X_GATHER, j, out_buf.at[0, place], out_buf.at[0, place], x_peer(o))
                send(l, X_GATHER, j, across, out_buf.at[0, place], x_cross(o))
            send(l, X_GATHER, j, across, out_buf.at[0, place], sibling)

    for i in range(12):
        loads[i].wait()
    pack_gate_up(0)
    pl.semaphore_wait(barrier, len(peers))
    for i in range(3):
        swaps[i].start()
    pack_scales(0)
    pack_scales(1)
    loads[12].wait()
    pack_down(0)
    swaps[3].start()
    for i in range(3):
        swaps[i].wait_recv()
    for j in range(chunks):
        gate_up(0, j)
    loads[13].wait()
    loads[14].wait()
    pack_gate_up(1)
    swaps[4].start()
    loads[15].wait()
    pack_down(1)
    swaps[5].start()
    for l in range(2):
        for j in range(chunks):
            if l == 1:
                await_recv(0, X_GATHER, j, acts.at[1, pl.ds(0, rows - x_rows)])
                if j == 0:
                    swaps[4].wait_recv()
                gate_up(1, j)
        for j in range(chunks):
            combine(l, j)
        for j in range(chunks):
            hidden(l, j)
        for j in range(chunks):
            forward(l, j)
        for j in range(chunks):
            if j == 0:
                swaps[3 + 2 * l].wait_recv()
            down(l, j)
        if l == 1:
            for j in range(chunks):
                await_send(0, X_SCATTER, j, down_in.at[0, j])
        for j in range(chunks):
            result(l, j)
    stores = []
    for j in range(chunks):
        await_recv(1, X_GATHER, j, out_buf.at[0, pl.ds(0, 2 * rows - x_rows)])
        for h in range(2):
            at = pl.ds(h * half + j * rows, rows)
            store = pltpu.make_async_copy(out_buf.at[0, at], out_hbm.at[at], out_sem.at[j, h])
            store.start()
            stores.append(store)
    for swap in swaps:
        swap.wait_send()
    for l in range(2):
        for j in range(chunks):
            await_send(l, SQUARES, j, sq_in.at[l, j])
            await_send(l, FOR_THREE, j, in_three.at[l, j])
            await_send(l, FOR_FOUR, j, in_four.at[l, j])
            await_send(l, FOR_ONE, j, in_one.at[l, j])
            await_send(l, FOR_TWO, j, in_two.at[l, j])
            await_send(l, FROM_TWO, j, hid.at[l, pl.ds(0, 2 * y_rows)])
            await_send(l, FROM_REST, j, hid.at[l, pl.ds(0, 5 * y_rows)])
            if l == 1:
                await_send(1, X_SCATTER, j, down_in.at[1, j])
                await_send(1, X_GATHER, j, out_buf.at[0, pl.ds(0, 2 * rows - x_rows)])
            else:
                await_send(0, X_GATHER, j, acts.at[1, pl.ds(0, rows - x_rows)])
    for store in stores:
        store.wait()


def local(n_y, n_x, *args):
    x, gate, down = args[0], args[2], args[6]
    tokens, width = x.shape
    ff = gate.shape[1]
    padded = ff // LANES * LANES + LANES
    half = tokens // 2
    rows = half // CHUNKS
    y_rows, x_rows = rows // n_y, rows // n_x
    flat = [a.reshape(1, -1) if a.shape == (width,) else a for a in args]
    for i in (2, 4, 9, 11):
        flat[i] = args[i].T
    dma = pltpu.SemaphoreType.DMA
    return pl.pallas_call(
        functools.partial(kernel, n_y, n_x, CHUNKS),
        name="half_steps",
        out_shape=jax.ShapeDtypeStruct(x.shape, x.dtype),
        in_specs=[pl.BlockSpec(memory_space=pl.ANY)] * len(flat),
        out_specs=pl.BlockSpec(memory_space=pl.ANY),
        scratch_shapes=[
            pltpu.VMEM((2, half, 2 * width), BF16),
            pltpu.VMEM((half, width), BF16),
            pltpu.VMEM((2, ff, width), F32),
            pltpu.VMEM((2, ff, width), F32),
            pltpu.VMEM((2, ff, width), F32),
            pltpu.VMEM((ff,), F32),
            pltpu.VMEM((ff,), F32),
            pltpu.VMEM((ff,), F32),
            pltpu.VMEM((ff,), F32),
            pltpu.VMEM((4, 1, width), F32),
            pltpu.VMEM((4, 1, width), F32),
            pltpu.VMEM((2, 2 * ff, 2 * width), BF16),
            pltpu.VMEM((2, padded, 2 * width), BF16),
            pltpu.VMEM((2, 1, 2 * ff), F32),
            pltpu.VMEM((2, half, 2 * ff), BF16),
            pltpu.VMEM((2, CHUNKS, 2, y_rows, 2 * ff), BF16),
            pltpu.VMEM((2, CHUNKS, y_rows, 2 * ff), BF16),
            pltpu.VMEM((2, CHUNKS, 2, y_rows, 2 * ff), BF16),
            pltpu.VMEM((2, CHUNKS, 2, y_rows, 2 * ff), BF16),
            pltpu.VMEM((2, CHUNKS, 2, y_rows, 2 * ff), BF16),
            pltpu.VMEM((2, CHUNKS, 1, rows), F32),
            pltpu.VMEM((2, CHUNKS, n_y - 1, 1, rows), F32),
            pltpu.VMEM((2, half, padded), BF16),
            pltpu.VMEM((2, half, 2 * width), BF16),
            pltpu.VMEM((2, CHUNKS, n_x - 1, x_rows, 2 * width), BF16),
            pltpu.VMEM((1, tokens, width), BF16),
            dma((16,)),
            dma((6,)),
            dma((6,)),
            dma((2, 9, CHUNKS)),
            dma((2, 9, CHUNKS)),
            dma((CHUNKS, 2)),
        ],
        compiler_params=pltpu.CompilerParams(collective_id=0, has_side_effects=True),
    )(*flat)


def solution(mesh):
    n_y, n_x = mesh.shape["ra"] // 2, mesh.shape["cb"]
    layer = (P("ra"), P("ra", "cb"), P("cb"), P("ra", "cb"), P("cb"), P("cb", "ra"), P("ra"))
    return jax.shard_map(
        functools.partial(local, n_y, n_x),
        mesh=mesh,
        in_specs=(P("grp", "ra"), *layer, *layer),
        out_specs=P("grp", "ra"),
        check_vma=False,
    )
```
